32 devices in a mesh: sp: 8 (over z, y), tp: 4 (over x, core).
Axes of the slice: x: 2, y: 2, z: 4, core: 2. Of those that a mesh axis runs over, the one named last changes fastest.
Arguments:
- tokens: bfloat16 [1024, 2048], P(('sp', 'tp')), may hold values from -64 to 64, as said below
- query_one: bfloat16 [2048, 256], P(None, 'tp'), may hold values from -0.125 to 0.125
- query_two: bfloat16 [2048, 256], P(None, 'tp'), may hold values from -0.125 to 0.125
- key_one: bfloat16 [2048, 256], P(None, 'tp'), may hold values from -0.125 to 0.125
- key_two: bfloat16 [2048, 256], P(None, 'tp'), may hold values from -0.125 to 0.125
- value_weight: bfloat16 [2048, 512], P(None, 'tp'), may hold values from -0.125 to 0.125
- mixing: float32 [4], P('tp'), may hold values from 0.3 to 0.8
- out_weight: bfloat16 [512, 2048], replicated, may hold values from -0.25 to 0.25
- head_gain: float32 [128], replicated, may hold values from 0.1 to 1.9
Outputs:
- attended: bfloat16 [1024, 2048], P(('sp', 'tp'))
The draws below stay inside these ranges and needn't reach their ends.
Inputs may be any that keep to these rules, and one draw needn't show every extreme that they name: `tokens`: Real-valued activations.
All inputs are finite; a program needn't handle non-finite values.
Results may differ from the reference program's by a relative error of at most 0.012.
The reference program's roundings to bfloat16 on the way count: a program that leaves them out, or rounds other values in their place, can miss the bound.
Values may be sent and summed in bfloat16 or wider, within the bound.
A program may use at most 64 MiB of HBM per device.

```python
import math
import jax
import jax.numpy as jnp
from jax import lax

D = 2048
HEADS = 4
HEAD = 64
GRID_W = 64
TOK_DEV = 128
TOKENS = 1024


def draw_tokens(key, part):
    key_base = jax.random.fold_in(key, 11)
    key_means = jax.random.fold_in(key, 12)
    blocks = TOKENS // TOK_DEV
    means = jnp.clip(jax.random.normal(key_means, (blocks, D), jnp.float32), -4.0, 4.0)
    spread_means = jnp.repeat(means, TOK_DEV, axis=0)
    base = jnp.clip(jax.random.normal(key_base, (TOKENS, D), jnp.float32), -4.0, 4.0)
    field = base + spread_means
    return jnp.clip(field, -64.0, 64.0).astype(jnp.bfloat16)


def level_of(rng, extent, shards, low, high):
    gain = 1.0
    for axis_at, parts in shards:
        heights = jax.random.uniform(jax.random.fold_in(jax.random.fold_in(rng, 6), axis_at), (parts,), jnp.float32, low / len(shards), high / len(shards))
        gain = gain * jnp.repeat(jnp.exp(heights), extent[axis_at] // parts).reshape((-1,) + (1,) * (len(extent) - 1 - axis_at))
    return gain


def bell_draw(stream_key, extent, width, reach, cuts=(), held_as=jnp.bfloat16):
    values = width * jax.random.normal(stream_key, extent, jnp.float32)
    if cuts:
        values = values * level_of(stream_key, extent, cuts, -0.22, 0.18)
    return jnp.clip(values, -reach, reach).astype(held_as)


def setup_inputs(seed: int = 0) -> dict:
    key_of = jax.random.split(jax.random.key(seed), 10)
    return {
        "tokens": draw_tokens(jax.random.fold_in(key_of[9], 71), 0),
        "query_one": bell_draw(key_of[1], (D, HEADS * HEAD), D ** -0.5, 0.125, ((1, 4),)),
        "query_two": bell_draw(key_of[2], (D, HEADS * HEAD), D ** -0.5, 0.125, ((1, 4),)),
        "key_one": bell_draw(key_of[3], (D, HEADS * HEAD), D ** -0.5, 0.125, ((1, 4),)),
        "key_two": bell_draw(key_of[4], (D, HEADS * HEAD), D ** -0.5, 0.125, ((1, 4),)),
        "value_weight": bell_draw(key_of[5], (D, HEADS * 2 * HEAD), D ** -0.5, 0.125, ((1, 4),)),
        "mixing": jnp.clip(0.3 + 0.5 * jax.random.uniform(key_of[6], (HEADS,), jnp.float32) ** level_of(key_of[6], (HEADS,), ((0, 4),), -0.2, 0.2), 0.3, 0.8),
        "out_weight": bell_draw(key_of[7], (HEADS * 2 * HEAD, D), (2 * HEADS * HEAD) ** -0.5, 0.25),
        "head_gain": jnp.clip(1.0 + 0.18 * jax.random.normal(key_of[8], (2 * HEAD,), jnp.float32), 0.1, 1.9),
    }


epsilon = 1e-06
theta_base = 10000.0

def grid_turn(field, positions):
    quarter = field.shape[-1] // 4
    half = 2 * quarter
    freqs = theta_base ** (-jnp.arange(quarter, dtype=jnp.float32) / quarter)
    row_angle = (positions // GRID_W).astype(jnp.float32)[:, None] * freqs
    col_angle = (positions % GRID_W).astype(jnp.float32)[:, None] * freqs

    def turn(segment, angle):
        cosine = jnp.cos(angle)[:, None, :]
        sine = jnp.sin(angle)[:, None, :]
        first = segment[..., :quarter]
        second = segment[..., quarter:]
        return jnp.concatenate([first * cosine - second * sine, first * sine + second * cosine], axis=-1)
    return jnp.concatenate([turn(field[..., :half], row_angle), turn(field[..., half:], col_angle)], axis=-1)

def project(tokens, weight):
    product = jnp.dot(tokens, weight, preferred_element_type=jnp.float32)
    return product.reshape(tokens.shape[0], HEADS, -1)

def reference(tokens, query_one, query_two, key_one, key_two, value_weight, mixing, out_weight, head_gain):
    positions = jnp.arange(TOKENS, dtype=jnp.int32)
    q_first = grid_turn(project(tokens, query_one), positions).astype(jnp.bfloat16)
    q_second = grid_turn(project(tokens, query_two), positions).astype(jnp.bfloat16)
    k_first = grid_turn(project(tokens, key_one), positions).astype(jnp.bfloat16).astype(jnp.float32)
    k_second = grid_turn(project(tokens, key_two), positions).astype(jnp.bfloat16).astype(jnp.float32)
    values = project(tokens, value_weight).astype(jnp.bfloat16).astype(jnp.float32)
    scale = HEAD ** (-0.5)
    block_rows = math.gcd(TOKENS, 256)

    def one_map(queries, keys):
        scores = jnp.einsum('qhd,khd->qhk', queries.astype(jnp.float32), keys) * scale
        peak = lax.optimization_barrier(jnp.max(scores, axis=-1, keepdims=True))
        weights = jnp.exp(scores - peak)
        total = lax.optimization_barrier(jnp.sum(weights, axis=-1))
        rounded = lax.optimization_barrier(weights.astype(jnp.bfloat16)).astype(jnp.float32)
        summed = jnp.einsum('qhk,khe->qhe', rounded, values)
        return summed / total[..., None]

    def attend(block):
        first_q, second_q = block
        mixed = one_map(first_q, k_first) - mixing[None, :, None] * one_map(second_q, k_second)
        normed = mixed * lax.rsqrt(lax.optimization_barrier(jnp.mean(mixed * mixed, axis=-1, keepdims=True)) + epsilon) * head_gain
        return normed.astype(jnp.bfloat16)
    count = TOKENS // block_rows
    heads = lax.map(attend, (q_first.reshape(count, block_rows, HEADS, HEAD), q_second.reshape(count, block_rows, HEADS, HEAD)))
    heads = heads.reshape(TOKENS, HEADS * 2 * HEAD)
    return jnp.dot(heads, out_weight, preferred_element_type=jnp.float32).astype(jnp.bfloat16)
```

```python
import functools
import math

import jax
import jax.numpy as jnp
from jax import lax
from jax.experimental import pallas as pl
from jax.experimental.pallas import tpu as pltpu
from jax.sharding import PartitionSpec as P

HEAD = 64
GRID_W = 64
QUARTER = HEAD // 4

epsilon = 1e-06
theta_base = 10000.0
floor_value = -1e30
MESH = pl.DeviceIdType.MESH
NT = (((1,), (1,)), ((), ()))
CHUNKS = 4


def rotary_tables(start, rows):
    shape = (rows, 2 * HEAD)
    lane = lax.broadcasted_iota(jnp.int32, shape, 1)
    token = lax.broadcasted_iota(jnp.int32, shape, 0) + start
    entry = lane % QUARTER
    freqs = jnp.zeros(shape, jnp.float32)
    for j in range(QUARTER):
        freqs = jnp.where(entry == j, jnp.float32(theta_base ** (-j / QUARTER)), freqs)
    by_row = (lane % HEAD) < 2 * QUARTER
    position = jnp.where(by_row, token // GRID_W, token % GRID_W).astype(jnp.float32)
    angle = position * freqs
    first = (lane % (2 * QUARTER)) < QUARTER
    sine = jnp.sin(angle)
    return jnp.cos(angle), jnp.where(first, -sine, sine)


def turn(field, cosine, sine):
    lane = lax.broadcasted_iota(jnp.int32, field.shape, 1)
    first = (lane % (2 * QUARTER)) < QUARTER
    width = field.shape[1]
    other = jnp.where(
        first, pltpu.roll(field, width - QUARTER, 1), pltpu.roll(field, QUARTER, 1)
    )
    return field * cosine + other * sine


def kernel(
    sp, tp,
    tokens, wq1, wq2, wk1, wk2, wv, mixing, wo, gain, out,
    tok, wqk, wvv, wov, tables, kv, hsend, hrecv,
    load_sems, tsend, trecv, fsend, frecv, ksend, krecv, hs_sems, hr_sems,
):
    own_rows, depth = tokens.shape
    rows = own_rows * tp
    groups = tp // 2
    me_tp = lax.axis_index("tp")
    me_sp = lax.axis_index("sp")
    partner = me_tp + 1 - 2 * (me_tp % 2)
    span = depth // CHUNKS

    tok_load = pltpu.make_async_copy(tokens, tok.at[me_tp], load_sems.at[0])
    tok_load.start()
    loads = []
    for i, w in enumerate((wq1, wq2, wk1, wk2)):
        loads.append(pltpu.make_async_copy(w, wqk.at[pl.ds(i * HEAD, HEAD)], load_sems.at[1 + i]))
    loads.append(pltpu.make_async_copy(wv, wvv, load_sems.at[5]))
    for c in loads:
        c.start()
    wo_load = pltpu.make_async_copy(wo, wov, load_sems.at[6])
    wo_load.start()

    barrier = pltpu.get_barrier_semaphore()
    for d in range(1, tp):
        pl.semaphore_signal(barrier, inc=1, device_id={"tp": lax.rem(me_tp + d, tp)}, device_id_type=MESH)

    def greet(d, _):
        pl.semaphore_signal(barrier, inc=1, device_id={"sp": lax.rem(me_sp + d, sp)}, device_id_type=MESH)
        return _

    lax.fori_loop(1, sp, greet, 0)
    pl.semaphore_wait(barrier, tp - 1 + sp - 1)

    def part(slot, c):
        return tok.at[slot, :, pl.ds(c * span, span)]

    def send(slot, c, target, s_sem, r_sem):
        return pltpu.make_async_remote_copy(
            src_ref=part(slot, c), dst_ref=part(slot, c), send_sem=s_sem, recv_sem=r_sem,
            device_id={"tp": target}, device_id_type=MESH,
        )

    def peer(g):
        return lax.rem(me_tp + 2 * g, tp)

    tok_load.wait()
    first_sends, forwards = [], []
    for c in range(CHUNKS):
        for g in range(1, groups):
            cp = send(me_tp, c, peer(g), tsend.at[g, c], trecv.at[g, c])
            cp.start()
            first_sends.append(cp)
        cp = send(me_tp, c, partner, tsend.at[0, c], trecv.at[0, c])
        cp.start()
        first_sends.append(cp)

    cosine, sine = rotary_tables(me_sp * rows, rows)
    tables[0] = cosine
    tables[1] = sine
    for c in loads:
        c.wait()

    acc_qk = jnp.zeros((rows, 4 * HEAD), jnp.float32)
    acc_v = jnp.zeros((rows, 2 * HEAD), jnp.float32)
    for c in range(CHUNKS):
        for g in range(1, groups):
            slot = lax.rem(me_tp + tp - 2 * g, tp)
            send(slot, c, partner, tsend.at[g, c], trecv.at[g, c]).wait_recv()
            cp = send(slot, c, partner, fsend.at[g, c], frecv.at[g, c])
            cp.start()
            forwards.append(cp)
        send(partner, c, partner, tsend.at[0, c], trecv.at[0, c]).wait_recv()
        for g in range(1, groups):
            slot = lax.rem(partner + tp - 2 * g, tp)
            send(slot, c, partner, fsend.at[g, c], frecv.at[g, c]).wait_recv()
        x = tok[:, :, c * span:(c + 1) * span].reshape(rows, span)
        acc_qk += lax.dot_general(x, wqk[:, c * span:(c + 1) * span], NT, preferred_element_type=jnp.float32)
        acc_v += jnp.dot(x, wvv[c * span:(c + 1) * span, :], preferred_element_type=jnp.float32)

    cosine, sine = tables[0], tables[1]
    keys = turn(acc_qk[:, 2 * HEAD:], cosine, sine).astype(jnp.bfloat16)
    kv[me_sp, :, : 2 * HEAD] = keys
    kv[me_sp, :, 2 * HEAD :] = acc_v.astype(jnp.bfloat16)

    def kv_copy(slot, d, target):
        return pltpu.make_async_remote_copy(
            src_ref=kv.at[slot], dst_ref=kv.at[slot], send_sem=ksend.at[d], recv_sem=krecv.at[d],
            device_id={"sp": target}, device_id_type=MESH,
        )

    def start_kv(d, _):
        kv_copy(me_sp, d, lax.rem(me_sp + d, sp)).start()
        return _

    lax.fori_loop(1, sp, start_kv, 0)

    queries = turn(acc_qk[:, : 2 * HEAD], cosine, sine)
    lane = lax.broadcasted_iota(jnp.int32, queries.shape, 1)
    both = jnp.concatenate(
        [jnp.where(lane < HEAD, queries, 0.0), jnp.where(lane < HEAD, 0.0, queries)], axis=0
    ).astype(jnp.bfloat16)

    def absorb(slot, state):
        peak, total, summed = state
        k = kv[slot, :, : 2 * HEAD]
        v = kv[slot, :, 2 * HEAD :]
        scores = lax.dot_general(both, k, NT, preferred_element_type=jnp.float32) * HEAD ** (-0.5)
        new_peak = jnp.maximum(peak, jnp.max(scores, axis=1, keepdims=True))
        factor = jnp.exp(peak - new_peak)
        weights = jnp.exp(scores - new_peak)
        total = total * factor + jnp.sum(weights, axis=1, keepdims=True)
        summed = summed * factor + jnp.dot(
            weights.astype(jnp.bfloat16), v, preferred_element_type=jnp.float32
        )
        return new_peak, total, summed

    state = (
        jnp.full((2 * rows, 1), floor_value, jnp.float32),
        jnp.zeros((2 * rows, 1), jnp.float32),
        jnp.zeros((2 * rows, 2 * HEAD), jnp.float32),
    )
    state = absorb(me_sp, state)

    def step(d, state):
        slot = lax.rem(me_sp + sp - d, sp)
        kv_copy(slot, d, slot).wait_recv()
        return absorb(slot, state)

    if sp <= 16:
        for d in range(1, sp):
            state = step(d, state)
    else:
        state = lax.fori_loop(1, sp, step, state)

    _, total, summed = state
    ratio = summed / total
    mixed = ratio[:rows] - mixing[0] * ratio[rows:]
    normed = (
        mixed * lax.rsqrt(jnp.mean(mixed * mixed, axis=-1, keepdims=True) + epsilon) * gain[...]
    )
    hsend[...] = normed.astype(jnp.bfloat16).reshape(tp, own_rows, 2 * HEAD)
    head_sends = []
    for d in range(1, tp):
        target = lax.rem(me_tp + d, tp)
        cp = pltpu.make_async_remote_copy(
            src_ref=hsend.at[target], dst_ref=hrecv.at[me_tp],
            send_sem=hs_sems.at[d], recv_sem=hr_sems.at[d],
            device_id={"tp": target}, device_id_type=MESH,
        )
        cp.start()
        head_sends.append(cp)
    hrecv[me_tp] = hsend[me_tp]
    wo_load.wait()
    for cp in head_sends:
        cp.wait_recv()
    joined = jnp.concatenate([hrecv[h] for h in range(tp)], axis=1)
    out[...] = jnp.dot(joined, wov[...], preferred_element_type=jnp.float32).astype(out.dtype)

    for cp in first_sends + forwards + head_sends:
        cp.wait_send()

    def drain(d, _):
        kv_copy(me_sp, d, lax.rem(me_sp + d, sp)).wait_send()
        return _

    lax.fori_loop(1, sp, drain, 0)


def per_device(
    sp, tp,
    tokens, query_one, query_two, key_one, key_two, value_weight, mixing, out_weight, head_gain
):
    own_rows, depth = tokens.shape
    rows = own_rows * tp
    assert query_one.shape[1] == HEAD
    any_spec = pl.BlockSpec(memory_space=pl.ANY)
    vmem = pl.BlockSpec(memory_space=pltpu.VMEM)
    dma = pltpu.SemaphoreType.DMA
    bf16 = jnp.bfloat16
    return pl.pallas_call(
        functools.partial(kernel, sp, tp),
        out_shape=jax.ShapeDtypeStruct((own_rows, out_weight.shape[1]), bf16),
        in_specs=[any_spec] * 6 + [pl.BlockSpec(memory_space=pltpu.SMEM), any_spec, vmem],
        out_specs=vmem,
        scratch_shapes=[
            pltpu.VMEM((tp, own_rows, depth), bf16),
            pltpu.VMEM((4 * HEAD, depth), bf16),
            pltpu.VMEM((depth, 2 * HEAD), bf16),
            pltpu.VMEM(out_weight.shape, bf16),
            pltpu.VMEM((2, rows, 2 * HEAD), jnp.float32),
            pltpu.VMEM((sp, rows, 4 * HEAD), bf16),
            pltpu.VMEM((tp, own_rows, 2 * HEAD), bf16),
            pltpu.VMEM((tp, own_rows, 2 * HEAD), bf16),
            dma((7,)),
            dma((tp // 2, CHUNKS)),
            dma((tp // 2, CHUNKS)),
            dma((tp // 2, CHUNKS)),
            dma((tp // 2, CHUNKS)),
            dma((sp,)),
            dma((sp,)),
            dma((tp,)),
            dma((tp,)),
        ],
        compiler_params=pltpu.CompilerParams(
            collective_id=0, has_side_effects=True, vmem_limit_bytes=56 * 1024 * 1024
        ),
    )(
        tokens, query_one.T, query_two.T, key_one.T, key_two.T, value_weight,
        mixing, out_weight, head_gain.reshape(1, -1),
    )


def solution(mesh):
    in_specs = (
        P(("sp", "tp"), None),
        P(None, "tp"),
        P(None, "tp"),
        P(None, "tp"),
        P(None, "tp"),
        P(None, "tp"),
        P("tp"),
        P(),
        P(),
    )
    out_specs = P(("sp", "tp"), None)
    return jax.shard_map(
        functools.partial(per_device, mesh.shape["sp"], mesh.shape["tp"]),
        mesh=mesh, in_specs=in_specs, out_specs=out_specs, check_vma=False,
    )
```

```python
import functools
import math

import jax
import jax.numpy as jnp
from jax import lax
from jax.experimental import pallas as pl
from jax.experimental.pallas import tpu as pltpu
from jax.sharding import PartitionSpec as P

HEAD = 64
GRID_W = 64
QUARTER = HEAD // 4

epsilon = 1e-06
theta_base = 10000.0
floor_value = -1e30
MESH = pl.DeviceIdType.MESH
NT = (((1,), (1,)), ((), ()))
CHUNKS = 4


def rotary_tables(start, rows):
    shape = (rows, 2 * HEAD)
    lane = lax.broadcasted_iota(jnp.int32, shape, 1)
    token = lax.broadcasted_iota(jnp.int32, shape, 0) + start
    entry = lane % QUARTER
    freqs = jnp.zeros(shape, jnp.float32)
    for j in range(QUARTER):
        freqs = jnp.where(entry == j, jnp.float32(theta_base ** (-j / QUARTER)), freqs)
    by_row = (lane % HEAD) < 2 * QUARTER
    position = jnp.where(by_row, token // GRID_W, token % GRID_W).astype(jnp.float32)
    angle = position * freqs
    first = (lane % (2 * QUARTER)) < QUARTER
    sine = jnp.sin(angle)
    return jnp.cos(angle), jnp.where(first, -sine, sine)


def turn(field, cosine, sine):
    lane = lax.broadcasted_iota(jnp.int32, field.shape, 1)
    first = (lane % (2 * QUARTER)) < QUARTER
    width = field.shape[1]
    other = jnp.where(
        first, pltpu.roll(field, width - QUARTER, 1), pltpu.roll(field, QUARTER, 1)
    )
    return field * cosine + other * sine


def kernel(
    sp, tp,
    tokens, wq1, wq2, wk1, wk2, wv, mixing, wo, gain, out,
    tok, wqk, wvv, wov, tables, kv, qbuf, hsend, hrecv,
    load_sems, tsend, trecv, fsend, frecv, ksend, krecv, hs_sems, hr_sems, ready,
):
    own_rows, depth = tokens.shape
    rows = own_rows * tp
    groups = tp // 2
    me_tp = lax.axis_index("tp")
    me_sp = lax.axis_index("sp")
    partner = me_tp + 1 - 2 * (me_tp % 2)
    span = depth // CHUNKS

    tok_load = pltpu.make_async_copy(tokens, tok.at[me_tp], load_sems.at[0])
    tok_load.start()
    loads = []
    for i, w in enumerate((wq1, wq2, wk1, wk2)):
        loads.append(pltpu.make_async_copy(w, wqk.at[pl.ds(i * HEAD, HEAD)], load_sems.at[1 + i]))
    loads.append(pltpu.make_async_copy(wv, wvv, load_sems.at[5]))
    for c in loads:
        c.start()
    wo_load = pltpu.make_async_copy(wo, wov, load_sems.at[6])
    wo_load.start()

    depth_z = sp // 2
    me_z = me_sp // 2
    side = me_sp + 1 - 2 * (me_sp % 2)
    barrier = pltpu.get_barrier_semaphore()
    has_left = jnp.minimum(me_z, 1)
    has_right = jnp.minimum(depth_z - 1 - me_z, 1)

    def signal_line(left_sem, right_sem):
        @pl.when(me_z > 0)
        def _():
            pl.semaphore_signal(right_sem, inc=1, device_id={"sp": me_sp - 2}, device_id_type=MESH)

        @pl.when(me_z < depth_z - 1)
        def _():
            pl.semaphore_signal(left_sem, inc=1, device_id={"sp": me_sp + 2}, device_id_type=MESH)

    for d in range(1, tp):
        pl.semaphore_signal(barrier, inc=1, device_id={"tp": lax.rem(me_tp + d, tp)}, device_id_type=MESH)
    pl.semaphore_signal(barrier, inc=1, device_id={"sp": side}, device_id_type=MESH)
    signal_line(barrier, barrier)
    pl.semaphore_wait(barrier, tp + has_left + has_right)

    def send(slot, c, target, s_sem, r_sem):
        part = tok.at[slot, :, pl.ds(c * span, span)]
        return pltpu.make_async_remote_copy(
            src_ref=part, dst_ref=part, send_sem=s_sem, recv_sem=r_sem,
            device_id={"tp": target}, device_id_type=MESH,
        )

    def send_whole(slot):
        return pltpu.make_async_remote_copy(
            src_ref=tok.at[slot], dst_ref=tok.at[slot], send_sem=tsend.at[0, 0], recv_sem=trecv.at[0, 0],
            device_id={"tp": partner}, device_id_type=MESH,
        )

    def peer(g):
        return lax.rem(me_tp + 2 * g, tp)

    tok_load.wait()
    first_sends, forwards = [], []
    cp = send_whole(me_tp)
    cp.start()
    first_sends.append(cp)
    for c in range(CHUNKS):
        for g in range(1, groups):
            cp = send(me_tp, c, peer(g), tsend.at[g, c], trecv.at[g, c])
            cp.start()
            first_sends.append(cp)

    cosine, sine = rotary_tables(me_sp * rows, rows)
    tables[0] = cosine
    tables[1] = sine

    def pass_on(_, carry):
        signal_line(ready.at[0], ready.at[1])

        @pl.when(me_z > 0)
        def _():
            pl.semaphore_wait(ready.at[0], 1)

        @pl.when(me_z < depth_z - 1)
        def _():
            pl.semaphore_wait(ready.at[1], 1)

        return carry

    if depth_z > 2:
        lax.fori_loop(0, depth_z - 2, pass_on, 0)
    for c in loads:
        c.wait()

    me_chip = me_tp // 2
    pair = 2 * own_rows

    def kv_copy(slot, chip, order, i, device):
        return pltpu.make_async_remote_copy(
            src_ref=kv.at[slot, chip], dst_ref=kv.at[slot, chip],
            send_sem=ksend.at[order, i], recv_sem=krecv.at[order, i],
            device_id={"sp": device}, device_id_type=MESH,
        )

    upper = (2 * me_z) // depth_z

    def distance(k):
        return upper * k + (1 - upper) * (depth_z - k)

    def along(d):
        return 2 * lax.rem(me_z + d, depth_z) + me_sp % 2

    def from_along(d):
        return 2 * lax.rem(me_z + depth_z - d, depth_z) + me_sp % 2

    def loop(count, body, state):
        if count <= 8:
            for k in range(1, count):
                state = body(k, state)
            return state
        return lax.fori_loop(1, count, body, state)

    def finish(chip, order, qk, values):
        cosine = tables[0, pl.ds(pl.multiple_of(chip * pair, pair), pair), :]
        sine = tables[1, pl.ds(pl.multiple_of(chip * pair, pair), pair), :]
        kv[me_sp, chip, :, : 2 * HEAD] = turn(qk[:, 2 * HEAD :], cosine, sine).astype(jnp.bfloat16)
        kv[me_sp, chip, :, 2 * HEAD :] = values.astype(jnp.bfloat16)

        def start(k, carry):
            d = distance(k)
            kv_copy(me_sp, chip, order, d, along(d)).start()
            return carry

        kv_copy(me_sp, chip, order, 0, side).start()
        loop(depth_z, start, 0)
        queries = turn(qk[:, : 2 * HEAD], cosine, sine)
        lane = lax.broadcasted_iota(jnp.int32, queries.shape, 1)
        qbuf[0, pl.ds(pl.multiple_of(chip * pair, pair), pair), :] = jnp.where(lane < HEAD, queries, 0.0).astype(jnp.bfloat16)
        qbuf[1, pl.ds(pl.multiple_of(chip * pair, pair), pair), :] = jnp.where(lane < HEAD, 0.0, queries).astype(jnp.bfloat16)

    def project(base, lower, size):
        x = tok[pl.ds(base, 2), :, lower : lower + size].reshape(pair, size)
        return (
            lax.dot_general(x, wqk[:, lower : lower + size], NT, preferred_element_type=jnp.float32),
            jnp.dot(x, wvv[lower : lower + size, :], preferred_element_type=jnp.float32),
        )

    send_whole(partner).wait_recv()
    finish(me_chip, 0, *project(2 * me_chip, 0, depth))
    for g in range(1, groups):
        chip = lax.rem(me_chip + groups - g, groups)
        slot = 2 * chip + me_tp % 2
        other = 2 * chip + partner % 2
        qk = jnp.zeros((pair, 4 * HEAD), jnp.float32)
        values = jnp.zeros((pair, 2 * HEAD), jnp.float32)
        for c in range(CHUNKS):
            send(slot, c, partner, tsend.at[g, c], trecv.at[g, c]).wait_recv()
            cp = send(slot, c, partner, fsend.at[g, c], frecv.at[g, c])
            cp.start()
            forwards.append(cp)
            send(other, c, partner, fsend.at[g, c], frecv.at[g, c]).wait_recv()
            more = project(2 * chip, c * span, span)
            qk += more[0]
            values += more[1]
        finish(chip, g, qk, values)

    both = qbuf[...].reshape(2 * rows, 2 * HEAD)

    def absorb(blocks, state):
        peak, total, summed = state
        block = jnp.concatenate([kv[slot, chip] for slot, chip in blocks], axis=0)
        k = block[:, : 2 * HEAD]
        v = block[:, 2 * HEAD :]
        scores = lax.dot_general(both, k, NT, preferred_element_type=jnp.float32) * HEAD ** (-0.5)
        new_peak = jnp.maximum(peak, jnp.max(scores, axis=1, keepdims=True))
        factor = jnp.exp(peak - new_peak)
        weights = jnp.exp(scores - new_peak)
        total = total * factor + jnp.sum(weights, axis=1, keepdims=True)
        summed = summed * factor + jnp.dot(
            weights.astype(jnp.bfloat16), v, preferred_element_type=jnp.float32
        )
        return new_peak, total, summed

    def absorb_line(sources, chip, also, state):
        if depth_z <= 8:
            return absorb([(sources(distance(k)), chip) for k in range(1, depth_z)] + also, state)
        if also:
            state = absorb(also, state)
        return lax.fori_loop(1, depth_z, lambda k, s: absorb([(sources(distance(k)), chip)], s), state)

    def side_of(d):
        slot = from_along(d)
        return slot + 1 - 2 * (slot % 2)

    state = (
        jnp.full((2 * rows, 1), floor_value, jnp.float32),
        jnp.zeros((2 * rows, 1), jnp.float32),
        jnp.zeros((2 * rows, 2 * HEAD), jnp.float32),
    )
    state = absorb([(me_sp, h) for h in range(groups)], state)

    def chip_of(order):
        return lax.rem(me_chip + groups - order, groups)

    def relay(order):
        chip = chip_of(order)

        def one(k, carry):
            d = distance(k)
            kv_copy(from_along(d), chip, order, d, side).wait_recv()
            kv_copy(from_along(d), chip, order, depth_z + d, side).start()
            return carry

        loop(depth_z, one, 0)

    def relayed(order):
        chip = chip_of(order)

        def one(k, carry):
            d = distance(k)
            kv_copy(side_of(d), chip, order, depth_z + d, side).wait_recv()
            return carry

        loop(depth_z, one, 0)

    for order in range(groups):
        chip = chip_of(order)
        relay(order)
        if order > 0:
            relayed(order - 1)
            state = absorb_line(side_of, chip_of(order - 1), [], state)
        kv_copy(side, chip, order, 0, side).wait_recv()
        state = absorb_line(from_along, chip, [(side, chip)], state)
    relayed(groups - 1)
    state = absorb_line(side_of, chip_of(groups - 1), [], state)

    _, total, summed = state
    ratio = summed / total
    mixed = ratio[:rows] - mixing[0] * ratio[rows:]
    normed = (
        mixed * lax.rsqrt(jnp.mean(mixed * mixed, axis=-1, keepdims=True) + epsilon) * gain[...]
    )
    hsend[...] = normed.astype(jnp.bfloat16).reshape(tp, own_rows, 2 * HEAD)
    head_sends = []
    for d in range(1, tp):
        target = lax.rem(me_tp + d, tp)
        cp = pltpu.make_async_remote_copy(
            src_ref=hsend.at[target], dst_ref=hrecv.at[me_tp],
            send_sem=hs_sems.at[d], recv_sem=hr_sems.at[d],
            device_id={"tp": target}, device_id_type=MESH,
        )
        cp.start()
        head_sends.append(cp)
    hrecv[me_tp] = hsend[me_tp]
    wo_load.wait()
    for cp in head_sends:
        cp.wait_recv()
    joined = jnp.concatenate([hrecv[h] for h in range(tp)], axis=1)
    out[...] = jnp.dot(joined, wov[...], preferred_element_type=jnp.float32).astype(out.dtype)

    for cp in first_sends + forwards + head_sends:
        cp.wait_send()

    for order in range(groups):

        def drain(i, carry):
            kv_copy(me_sp, 0, order, i, side).wait_send()
            return carry

        lax.fori_loop(0, depth_z, drain, 0)
        lax.fori_loop(depth_z + 1, 2 * depth_z, drain, 0)


def per_device(
    sp, tp,
    tokens, query_one, query_two, key_one, key_two, value_weight, mixing, out_weight, head_gain
):
    own_rows, depth = tokens.shape
    rows = own_rows * tp
    assert query_one.shape[1] == HEAD
    any_spec = pl.BlockSpec(memory_space=pl.ANY)
    vmem = pl.BlockSpec(memory_space=pltpu.VMEM)
    dma = pltpu.SemaphoreType.DMA
    bf16 = jnp.bfloat16
    return pl.pallas_call(
        functools.partial(kernel, sp, tp),
        out_shape=jax.ShapeDtypeStruct((own_rows, out_weight.shape[1]), bf16),
        in_specs=[any_spec] * 6 + [pl.BlockSpec(memory_space=pltpu.SMEM), any_spec, vmem],
        out_specs=vmem,
        scratch_shapes=[
            pltpu.VMEM((tp, own_rows, depth), bf16),
            pltpu.VMEM((4 * HEAD, depth), bf16),
            pltpu.VMEM((depth, 2 * HEAD), bf16),
            pltpu.VMEM(out_weight.shape, bf16),
            pltpu.VMEM((2, rows, 2 * HEAD), jnp.float32),
            pltpu.VMEM((sp, tp // 2, 2 * own_rows, 4 * HEAD), bf16),
            pltpu.VMEM((2, rows, 2 * HEAD), bf16),
            pltpu.VMEM((tp, own_rows, 2 * HEAD), bf16),
            pltpu.VMEM((tp, own_rows, 2 * HEAD), bf16),
            dma((7,)),
            dma((tp // 2, CHUNKS)),
            dma((tp // 2, CHUNKS)),
            dma((tp // 2, CHUNKS)),
            dma((tp // 2, CHUNKS)),
            dma((tp // 2, sp)),
            dma((tp // 2, sp)),
            dma((tp,)),
            dma((tp,)),
            pltpu.SemaphoreType.REGULAR((2,)),
        ],
        compiler_params=pltpu.CompilerParams(
            collective_id=0, has_side_effects=True, vmem_limit_bytes=56 * 1024 * 1024
        ),
    )(
        tokens, query_one.T, query_two.T, key_one.T, key_two.T, value_weight,
        mixing, out_weight, head_gain.reshape(1, -1),
    )


def solution(mesh):
    in_specs = (
        P(("sp", "tp"), None),
        P(None, "tp"),
        P(None, "tp"),
        P(None, "tp"),
        P(None, "tp"),
        P(None, "tp"),
        P("tp"),
        P(),
        P(),
    )
    out_specs = P(("sp", "tp"), None)
    return jax.shard_map(
        functools.partial(per_device, mesh.shape["sp"], mesh.shape["tp"]),
        mesh=mesh, in_specs=in_specs, out_specs=out_specs, check_vma=False,
    )
```

```python
import functools
import math

import jax
import jax.numpy as jnp
from jax import lax
from jax.experimental import pallas as pl
from jax.experimental.pallas import tpu as pltpu
from jax.sharding import PartitionSpec as P

HEAD = 64
GRID_W = 64
QUARTER = HEAD // 4

epsilon = 1e-06
theta_base = 10000.0
floor_value = -1e30
MESH = pl.DeviceIdType.MESH
NT = (((1,), (1,)), ((), ()))
CHUNKS = 4


def rotary_tables(start, rows):
    shape = (rows, 2 * HEAD)
    lane = lax.broadcasted_iota(jnp.int32, shape, 1)
    token = lax.broadcasted_iota(jnp.int32, shape, 0) + start
    entry = lane % QUARTER
    freqs = jnp.zeros(shape, jnp.float32)
    for j in range(QUARTER):
        freqs = jnp.where(entry == j, jnp.float32(theta_base ** (-j / QUARTER)), freqs)
    by_row = (lane % HEAD) < 2 * QUARTER
    position = jnp.where(by_row, token // GRID_W, token % GRID_W).astype(jnp.float32)
    angle = position * freqs
    first = (lane % (2 * QUARTER)) < QUARTER
    sine = jnp.sin(angle)
    return jnp.cos(angle), jnp.where(first, -sine, sine)


def turn(field, cosine, sine):
    lane = lax.broadcasted_iota(jnp.int32, field.shape, 1)
    first = (lane % (2 * QUARTER)) < QUARTER
    width = field.shape[1]
    other = jnp.where(
        first, pltpu.roll(field, width - QUARTER, 1), pltpu.roll(field, QUARTER, 1)
    )
    return field * cosine + other * sine


def kernel(
    sp, tp,
    tokens, wq1, wq2, wk1, wk2, wv, mixing, wo, gain, out,
    tok, wqk, wvv, wov, tables, kv, qbuf, hsend, hrecv,
    load_sems, tsend, trecv, fsend, frecv, ksend, krecv, hs_sems, hr_sems, ready, mix_in, gain_in,
):
    own_rows, depth = tokens.shape
    rows = own_rows * tp
    groups = tp // 2
    me_tp = lax.axis_index("tp")
    me_sp = lax.axis_index("sp")
    partner = me_tp + 1 - 2 * (me_tp % 2)
    span = depth // CHUNKS

    depth_z = sp // 2
    me_z = me_sp // 2
    side = me_sp + 1 - 2 * (me_sp % 2)
    barrier = pltpu.get_barrier_semaphore()
    has_left = jnp.minimum(me_z, 1)
    has_right = jnp.minimum(depth_z - 1 - me_z, 1)

    def signal_line(left_sem, right_sem):
        @pl.when(me_z > 0)
        def _():
            pl.semaphore_signal(right_sem, inc=1, device_id={"sp": me_sp - 2}, device_id_type=MESH)

        @pl.when(me_z < depth_z - 1)
        def _():
            pl.semaphore_signal(left_sem, inc=1, device_id={"sp": me_sp + 2}, device_id_type=MESH)

    for d in range(1, tp):
        pl.semaphore_signal(barrier, inc=1, device_id={"tp": lax.rem(me_tp + d, tp)}, device_id_type=MESH)
    pl.semaphore_signal(barrier, inc=1, device_id={"sp": side}, device_id_type=MESH)
    signal_line(barrier, barrier)
    tok_load = pltpu.make_async_copy(tokens, tok.at[me_tp], load_sems.at[0])
    tok_load.start()
    loads = []
    for i, w in enumerate((wq1, wq2, wk1, wk2)):
        loads.append(pltpu.make_async_copy(w, wqk.at[pl.ds(i * HEAD, HEAD)], load_sems.at[1 + i]))
    loads.append(pltpu.make_async_copy(wv, wvv, load_sems.at[5]))
    for c in loads:
        c.start()
    wo_load = pltpu.make_async_copy(wo, wov, load_sems.at[6])
    wo_load.start()
    small = [
        pltpu.make_async_copy(mixing, mix_in, load_sems.at[7]),
        pltpu.make_async_copy(gain, gain_in, load_sems.at[8]),
    ]
    for c in small:
        c.start()

    pl.semaphore_wait(barrier, tp + has_left + has_right)

    def send(slot, c, target, s_sem, r_sem):
        part = tok.at[slot, :, pl.ds(c * span, span)]
        return pltpu.make_async_remote_copy(
            src_ref=part, dst_ref=part, send_sem=s_sem, recv_sem=r_sem,
            device_id={"tp": target}, device_id_type=MESH,
        )

    def send_whole(slot):
        return pltpu.make_async_remote_copy(
            src_ref=tok.at[slot], dst_ref=tok.at[slot], send_sem=tsend.at[0, 0], recv_sem=trecv.at[0, 0],
            device_id={"tp": partner}, device_id_type=MESH,
        )

    def peer(g):
        return lax.rem(me_tp + 2 * g, tp)

    tok_load.wait()
    first_sends, forwards = [], []
    cp = send_whole(me_tp)
    cp.start()
    first_sends.append(cp)
    for c in range(CHUNKS):
        for g in range(1, groups):
            cp = send(me_tp, c, peer(g), tsend.at[g, c], trecv.at[g, c])
            cp.start()
            first_sends.append(cp)

    cosine, sine = rotary_tables(me_sp * rows, rows)
    tables[0] = cosine
    tables[1] = sine

    def pass_on(_, carry):
        signal_line(ready.at[0], ready.at[1])

        @pl.when(me_z > 0)
        def _():
            pl.semaphore_wait(ready.at[0], 1)

        @pl.when(me_z < depth_z - 1)
        def _():
            pl.semaphore_wait(ready.at[1], 1)

        return carry

    if depth_z > 2:
        lax.fori_loop(0, depth_z - 2, pass_on, 0)
    for c in loads + small + [wo_load]:
        c.wait()

    me_chip = me_tp // 2
    pair = 2 * own_rows

    def kv_copy(slot, chip, order, i, device):
        return pltpu.make_async_remote_copy(
            src_ref=kv.at[slot, chip], dst_ref=kv.at[slot, chip],
            send_sem=ksend.at[order, i], recv_sem=krecv.at[order, i],
            device_id={"sp": device}, device_id_type=MESH,
        )

    upper = (2 * me_z) // depth_z

    def distance(k):
        return upper * k + (1 - upper) * (depth_z - k)

    def along(d):
        return 2 * lax.rem(me_z + d, depth_z) + me_sp % 2

    def from_along(d):
        return 2 * lax.rem(me_z + depth_z - d, depth_z) + me_sp % 2

    def loop(count, body, state):
        if count <= 8:
            for k in range(1, count):
                state = body(k, state)
            return state
        return lax.fori_loop(1, count, body, state)

    def finish(chip, order, qk, values):
        cosine = tables[0, pl.ds(pl.multiple_of(chip * pair, pair), pair), :]
        sine = tables[1, pl.ds(pl.multiple_of(chip * pair, pair), pair), :]
        kv[me_sp, chip, :, : 2 * HEAD] = turn(qk[:, 2 * HEAD :], cosine, sine).astype(jnp.bfloat16)
        kv[me_sp, chip, :, 2 * HEAD :] = values.astype(jnp.bfloat16)

        def start(k, carry):
            d = distance(k)
            kv_copy(me_sp, chip, order, d, along(d)).start()
            return carry

        kv_copy(me_sp, chip, order, 0, side).start()
        loop(depth_z, start, 0)
        queries = turn(qk[:, : 2 * HEAD], cosine, sine)
        lane = lax.broadcasted_iota(jnp.int32, queries.shape, 1)
        qbuf[0, pl.ds(pl.multiple_of(chip * pair, pair), pair), :] = jnp.where(lane < HEAD, queries, 0.0).astype(jnp.bfloat16)
        qbuf[1, pl.ds(pl.multiple_of(chip * pair, pair), pair), :] = jnp.where(lane < HEAD, 0.0, queries).astype(jnp.bfloat16)

    def project(base, lower, size):
        x = tok[pl.ds(base, 2), :, lower : lower + size].reshape(pair, size)
        return (
            lax.dot_general(x, wqk[:, lower : lower + size], NT, preferred_element_type=jnp.float32),
            jnp.dot(x, wvv[lower : lower + size, :], preferred_element_type=jnp.float32),
        )

    send_whole(partner).wait_recv()
    finish(me_chip, 0, *project(2 * me_chip, 0, depth))
    for g in range(1, groups):
        chip = lax.rem(me_chip + groups - g, groups)
        slot = 2 * chip + me_tp % 2
        other = 2 * chip + partner % 2
        qk = jnp.zeros((pair, 4 * HEAD), jnp.float32)
        values = jnp.zeros((pair, 2 * HEAD), jnp.float32)
        for c in range(CHUNKS):
            send(slot, c, partner, tsend.at[g, c], trecv.at[g, c]).wait_recv()
            cp = send(slot, c, partner, fsend.at[g, c], frecv.at[g, c])
            cp.start()
            forwards.append(cp)
            send(other, c, partner, fsend.at[g, c], frecv.at[g, c]).wait_recv()
            more = project(2 * chip, c * span, span)
            qk += more[0]
            values += more[1]
        finish(chip, g, qk, values)

    both = qbuf[...].reshape(2 * rows, 2 * HEAD)

    def absorb(blocks, state):
        peak, total, summed = state
        block = jnp.concatenate([kv[slot, chip] for slot, chip in blocks], axis=0)
        k = block[:, : 2 * HEAD]
        v = block[:, 2 * HEAD :]
        scores = lax.dot_general(both, k, NT, preferred_element_type=jnp.float32) * HEAD ** (-0.5)
        new_peak = jnp.maximum(peak, jnp.max(scores, axis=1, keepdims=True))
        factor = jnp.exp(peak - new_peak)
        weights = jnp.exp(scores - new_peak)
        total = total * factor + jnp.sum(weights, axis=1, keepdims=True)
        summed = summed * factor + jnp.dot(
            weights.astype(jnp.bfloat16), v, preferred_element_type=jnp.float32
        )
        return new_peak, total, summed

    def absorb_line(sources, chip, also, state):
        if depth_z <= 8:
            return absorb([(sources(distance(k)), chip) for k in range(1, depth_z)] + also, state)
        if also:
            state = absorb(also, state)
        return lax.fori_loop(1, depth_z, lambda k, s: absorb([(sources(distance(k)), chip)], s), state)

    def side_of(d):
        slot = from_along(d)
        return slot + 1 - 2 * (slot % 2)

    state = (
        jnp.full((2 * rows, 1), floor_value, jnp.float32),
        jnp.zeros((2 * rows, 1), jnp.float32),
        jnp.zeros((2 * rows, 2 * HEAD), jnp.float32),
    )
    state = absorb([(me_sp, h) for h in range(groups)], state)

    def chip_of(order):
        return lax.rem(me_chip + groups - order, groups)

    def relay(order):
        chip = chip_of(order)

        def one(k, carry):
            d = distance(k)
            kv_copy(from_along(d), chip, order, d, side).wait_recv()
            kv_copy(from_along(d), chip, order, depth_z + d, side).start()
            return carry

        loop(depth_z, one, 0)

    def relayed(order):
        chip = chip_of(order)

        def one(k, carry):
            d = distance(k)
            kv_copy(side_of(d), chip, order, depth_z + d, side).wait_recv()
            return carry

        loop(depth_z, one, 0)

    for order in range(groups):
        chip = chip_of(order)
        relay(order)
        if order > 0:
            relayed(order - 1)
            state = absorb_line(side_of, chip_of(order - 1), [], state)
        kv_copy(side, chip, order, 0, side).wait_recv()
        state = absorb_line(from_along, chip, [(side, chip)], state)
    relayed(groups - 1)
    state = absorb_line(side_of, chip_of(groups - 1), [], state)

    _, total, summed = state
    ratio = summed / total
    mixed = ratio[:rows] - mix_in[...] * ratio[rows:]
    normed = (
        mixed * lax.rsqrt(jnp.mean(mixed * mixed, axis=-1, keepdims=True) + epsilon) * gain_in[...]
    )
    hsend[...] = normed.astype(jnp.bfloat16).reshape(tp, own_rows, 2 * HEAD)
    head_sends = []
    for d in range(1, tp):
        target = lax.rem(me_tp + d, tp)
        cp = pltpu.make_async_remote_copy(
            src_ref=hsend.at[target], dst_ref=hrecv.at[me_tp],
            send_sem=hs_sems.at[d], recv_sem=hr_sems.at[d],
            device_id={"tp": target}, device_id_type=MESH,
        )
        cp.start()
        head_sends.append(cp)
    hrecv[me_tp] = hsend[me_tp]
    for cp in head_sends:
        cp.wait_recv()
    joined = jnp.concatenate([hrecv[h] for h in range(tp)], axis=1)
    out[...] = jnp.dot(joined, wov[...], preferred_element_type=jnp.float32).astype(out.dtype)

    for cp in first_sends + forwards + head_sends:
        cp.wait_send()

    for order in range(groups):

        def drain(i, carry):
            kv_copy(me_sp, 0, order, i, side).wait_send()
            return carry

        lax.fori_loop(0, depth_z, drain, 0)
        lax.fori_loop(depth_z + 1, 2 * depth_z, drain, 0)


def per_device(
    sp, tp,
    tokens, query_one, query_two, key_one, key_two, value_weight, mixing, out_weight, head_gain
):
    own_rows, depth = tokens.shape
    rows = own_rows * tp
    assert query_one.shape[1] == HEAD
    any_spec = pl.BlockSpec(memory_space=pl.ANY)
    vmem = pl.BlockSpec(memory_space=pltpu.VMEM)
    dma = pltpu.SemaphoreType.DMA
    bf16 = jnp.bfloat16
    return pl.pallas_call(
        functools.partial(kernel, sp, tp),
        out_shape=pltpu.VMEM((own_rows, out_weight.shape[1]), bf16),
        in_specs=[any_spec] * 6 + [any_spec] * 3,
        out_specs=vmem,
        scratch_shapes=[
            pltpu.VMEM((tp, own_rows, depth), bf16),
            pltpu.VMEM((4 * HEAD, depth), bf16),
            pltpu.VMEM((depth, 2 * HEAD), bf16),
            pltpu.VMEM(out_weight.shape, bf16),
            pltpu.VMEM((2, rows, 2 * HEAD), jnp.float32),
            pltpu.VMEM((sp, tp // 2, 2 * own_rows, 4 * HEAD), bf16),
            pltpu.VMEM((2, rows, 2 * HEAD), bf16),
            pltpu.VMEM((tp, own_rows, 2 * HEAD), bf16),
            pltpu.VMEM((tp, own_rows, 2 * HEAD), bf16),
            dma((9,)),
            dma((tp // 2, CHUNKS)),
            dma((tp // 2, CHUNKS)),
            dma((tp // 2, CHUNKS)),
            dma((tp // 2, CHUNKS)),
            dma((tp // 2, sp)),
            dma((tp // 2, sp)),
            dma((tp,)),
            dma((tp,)),
            pltpu.SemaphoreType.REGULAR((2,)),
            pltpu.VMEM((1, 1), jnp.float32),
            pltpu.VMEM((1, 2 * HEAD), jnp.float32),
        ],
        compiler_params=pltpu.CompilerParams(
            collective_id=0, has_side_effects=True, vmem_limit_bytes=56 * 1024 * 1024
        ),
    )(
        tokens, query_one.T, query_two.T, key_one.T, key_two.T, value_weight,
        mixing.reshape(1, 1), out_weight, head_gain.reshape(1, -1),
    )


def solution(mesh):
    in_specs = (
        P(("sp", "tp"), None),
        P(None, "tp"),
        P(None, "tp"),
        P(None, "tp"),
        P(None, "tp"),
        P(None, "tp"),
        P("tp"),
        P(),
        P(),
    )
    out_specs = P(("sp", "tp"), None)
    return jax.shard_map(
        functools.partial(per_device, mesh.shape["sp"], mesh.shape["tp"]),
        mesh=mesh, in_specs=in_specs, out_specs=out_specs, check_vma=False,
    )
```

```python
import functools
import math

import jax
import jax.numpy as jnp
from jax import lax
from jax.experimental import pallas as pl
from jax.experimental.pallas import tpu as pltpu
from jax.sharding import PartitionSpec as P

HEAD = 64
GRID_W = 64
QUARTER = HEAD // 4

epsilon = 1e-06
theta_base = 10000.0
floor_value = -1e30
MESH = pl.DeviceIdType.MESH
NT = (((1,), (1,)), ((), ()))
PIECES = 2


def rotary_tables(start, rows, own_rows):
    shape = (rows, 2 * HEAD)
    lane = lax.broadcasted_iota(jnp.int32, shape, 1)
    index = lax.broadcasted_iota(jnp.int32, shape, 0)
    half = own_rows // PIECES
    device = 2 * (index // (2 * own_rows)) + (index % own_rows) // half
    piece = (index % (2 * own_rows)) // own_rows
    token = start + device * own_rows + piece * half + index % half
    entry = lane % QUARTER
    freqs = jnp.zeros(shape, jnp.float32)
    for j in range(QUARTER):
        freqs = jnp.where(entry == j, jnp.float32(theta_base ** (-j / QUARTER)), freqs)
    by_row = (lane % HEAD) < 2 * QUARTER
    position = jnp.where(by_row, token // GRID_W, token % GRID_W).astype(jnp.float32)
    angle = position * freqs
    first = (lane % (2 * QUARTER)) < QUARTER
    sine = jnp.sin(angle)
    return jnp.cos(angle), jnp.where(first, -sine, sine)


def turn(field, cosine, sine):
    lane = lax.broadcasted_iota(jnp.int32, field.shape, 1)
    first = (lane % (2 * QUARTER)) < QUARTER
    width = field.shape[1]
    other = jnp.where(
        first, pltpu.roll(field, width - QUARTER, 1), pltpu.roll(field, QUARTER, 1)
    )
    return field * cosine + other * sine


def kernel(
    sp, tp,
    tokens, wq1, wq2, wk1, wk2, wv, mixing, wo, gain, out,
    tok, wqk, wvv, wov, tables, kv, qbuf, hsend, hrecv,
    load_sems, tsend, trecv, fsend, frecv, ksend, krecv, hs_sems, hr_sems, ready, mix_in, gain_in,
):
    own_rows, depth = tokens.shape
    rows = own_rows * tp
    groups = tp // 2
    me_tp = lax.axis_index("tp")
    me_sp = lax.axis_index("sp")
    partner = me_tp + 1 - 2 * (me_tp % 2)
    half = own_rows // PIECES
    pair = 2 * own_rows
    me_chip = me_tp // 2
    orders = [(0, None)] + [(g, r) for g in range(1, groups) for r in range(PIECES)]

    depth_z = sp // 2
    me_z = me_sp // 2
    side = me_sp + 1 - 2 * (me_sp % 2)
    barrier = pltpu.get_barrier_semaphore()
    has_left = jnp.minimum(me_z, 1)
    has_right = jnp.minimum(depth_z - 1 - me_z, 1)

    def signal_line(left_sem, right_sem):
        @pl.when(me_z > 0)
        def _():
            pl.semaphore_signal(right_sem, inc=1, device_id={"sp": me_sp - 2}, device_id_type=MESH)

        @pl.when(me_z < depth_z - 1)
        def _():
            pl.semaphore_signal(left_sem, inc=1, device_id={"sp": me_sp + 2}, device_id_type=MESH)

    for d in range(1, tp):
        pl.semaphore_signal(barrier, inc=1, device_id={"tp": lax.rem(me_tp + d, tp)}, device_id_type=MESH)
    pl.semaphore_signal(barrier, inc=1, device_id={"sp": side}, device_id_type=MESH)
    signal_line(barrier, barrier)
    tok_load = pltpu.make_async_copy(tokens, tok.at[me_tp], load_sems.at[0])
    tok_load.start()
    loads = []
    for i, w in enumerate((wq1, wq2, wk1, wk2)):
        loads.append(pltpu.make_async_copy(w, wqk.at[pl.ds(i * HEAD, HEAD)], load_sems.at[1 + i]))
    loads.append(pltpu.make_async_copy(wv, wvv, load_sems.at[5]))
    for c in loads:
        c.start()
    wo_load = pltpu.make_async_copy(wo, wov, load_sems.at[6])
    wo_load.start()
    small = [
        pltpu.make_async_copy(mixing, mix_in, load_sems.at[7]),
        pltpu.make_async_copy(gain, gain_in, load_sems.at[8]),
    ]
    for c in small:
        c.start()

    pl.semaphore_wait(barrier, tp + has_left + has_right)

    def send(slot, c, target, s_sem, r_sem):
        part = tok.at[slot, pl.ds(c * half, half)]
        return pltpu.make_async_remote_copy(
            src_ref=part, dst_ref=part, send_sem=s_sem, recv_sem=r_sem,
            device_id={"tp": target}, device_id_type=MESH,
        )

    def send_whole(slot):
        return pltpu.make_async_remote_copy(
            src_ref=tok.at[slot], dst_ref=tok.at[slot], send_sem=tsend.at[0, 0], recv_sem=trecv.at[0, 0],
            device_id={"tp": partner}, device_id_type=MESH,
        )

    def peer(g):
        return lax.rem(me_tp + 2 * g, tp)

    tok_load.wait()
    first_sends, forwards = [], []
    cp = send_whole(me_tp)
    cp.start()
    first_sends.append(cp)
    for c in range(PIECES):
        for g in range(1, groups):
            cp = send(me_tp, c, peer(g), tsend.at[g, c], trecv.at[g, c])
            cp.start()
            first_sends.append(cp)

    cosine, sine = rotary_tables(me_sp * rows, rows, own_rows)
    tables[0] = cosine
    tables[1] = sine

    def pass_on(_, carry):
        signal_line(ready.at[0], ready.at[1])

        @pl.when(me_z > 0)
        def _():
            pl.semaphore_wait(ready.at[0], 1)

        @pl.when(me_z < depth_z - 1)
        def _():
            pl.semaphore_wait(ready.at[1], 1)

        return carry

    if depth_z > 2:
        lax.fori_loop(0, depth_z - 2, pass_on, 0)
    for c in loads + small + [wo_load]:
        c.wait()

    def chip_of(order):
        return lax.rem(me_chip + groups - orders[order][0], groups)

    def held(slot, order):
        piece = orders[order][1]
        if piece is None:
            return kv.at[slot, chip_of(order)]
        return kv.at[slot, chip_of(order), piece]

    def kv_copy(slot, order, i, device):
        return pltpu.make_async_remote_copy(
            src_ref=held(slot, order), dst_ref=held(slot, order),
            send_sem=ksend.at[order, i], recv_sem=krecv.at[order, i],
            device_id={"sp": device}, device_id_type=MESH,
        )

    upper = (2 * me_z) // depth_z

    def distance(k):
        return upper * k + (1 - upper) * (depth_z - k)

    def along(d):
        return 2 * lax.rem(me_z + d, depth_z) + me_sp % 2

    def from_along(d):
        return 2 * lax.rem(me_z + depth_z - d, depth_z) + me_sp % 2

    def loop(count, body, state):
        if count <= 8:
            for k in range(1, count):
                state = body(k, state)
            return state
        return lax.fori_loop(1, count, body, state)

    def finish(order):
        chip = chip_of(order)
        piece = orders[order][1]
        pieces = range(PIECES) if piece is None else (piece,)
        x = jnp.concatenate(
            [
                tok[pl.ds(2 * chip, 2), r * half : (r + 1) * half, :].reshape(own_rows, depth)
                for r in pieces
            ],
            axis=0,
        )
        count = x.shape[0]
        qk = lax.dot_general(x, wqk[...], NT, preferred_element_type=jnp.float32)
        values = jnp.dot(x, wvv[...], preferred_element_type=jnp.float32)
        start = pl.multiple_of(chip * pair + pieces[0] * own_rows, own_rows)
        where = pl.ds(start, count)
        cosine = tables[0, where, :]
        sine = tables[1, where, :]
        keys = turn(qk[:, 2 * HEAD :], cosine, sine).astype(jnp.bfloat16)
        values = values.astype(jnp.bfloat16)
        for i, r in enumerate(pieces):
            kv[me_sp, chip, r, :, : 2 * HEAD] = keys[i * own_rows : (i + 1) * own_rows]
            kv[me_sp, chip, r, :, 2 * HEAD :] = values[i * own_rows : (i + 1) * own_rows]

        def start_line(k, carry):
            d = distance(k)
            kv_copy(me_sp, order, d, along(d)).start()
            return carry

        loop(depth_z, start_line, 0)
        kv_copy(me_sp, order, 0, side).start()
        queries = turn(qk[:, : 2 * HEAD], cosine, sine)
        lane = lax.broadcasted_iota(jnp.int32, queries.shape, 1)
        qbuf[0, where, :] = jnp.where(lane < HEAD, queries, 0.0).astype(jnp.bfloat16)
        qbuf[1, where, :] = jnp.where(lane < HEAD, 0.0, queries).astype(jnp.bfloat16)

    send_whole(partner).wait_recv()
    finish(0)
    for order in range(1, len(orders)):
        g, r = orders[order]
        slot = 2 * chip_of(order) + me_tp % 2
        other = 2 * chip_of(order) + partner % 2
        send(slot, r, partner, tsend.at[g, r], trecv.at[g, r]).wait_recv()
        cp = send(slot, r, partner, fsend.at[g, r], frecv.at[g, r])
        cp.start()
        forwards.append(cp)
        send(other, r, partner, fsend.at[g, r], frecv.at[g, r]).wait_recv()
        finish(order)

    both = qbuf[...].reshape(2 * rows, 2 * HEAD)

    def absorb(blocks, state):
        peak, total, summed = state
        block = jnp.concatenate([b[...].reshape(-1, 4 * HEAD) for b in blocks], axis=0)
        k = block[:, : 2 * HEAD]
        v = block[:, 2 * HEAD :]
        scores = lax.dot_general(both, k, NT, preferred_element_type=jnp.float32) * HEAD ** (-0.5)
        new_peak = jnp.maximum(peak, jnp.max(scores, axis=1, keepdims=True))
        factor = jnp.exp(peak - new_peak)
        weights = jnp.exp(scores - new_peak)
        total = total * factor + jnp.sum(weights, axis=1, keepdims=True)
        summed = summed * factor + jnp.dot(
            weights.astype(jnp.bfloat16), v, preferred_element_type=jnp.float32
        )
        return new_peak, total, summed

    def absorb_line(sources, order, also, state):
        if depth_z <= 8:
            line = [held(sources(distance(k)), order) for k in range(1, depth_z)]
            return absorb(line + also, state)
        if also:
            state = absorb(also, state)
        return lax.fori_loop(
            1, depth_z, lambda k, s: absorb([held(sources(distance(k)), order)], s), state
        )

    def side_of(d):
        slot = from_along(d)
        return slot + 1 - 2 * (slot % 2)

    state = (
        jnp.full((2 * rows, 1), floor_value, jnp.float32),
        jnp.zeros((2 * rows, 1), jnp.float32),
        jnp.zeros((2 * rows, 2 * HEAD), jnp.float32),
    )
    state = absorb([kv.at[me_sp]], state)

    def relay(order):
        def one(k, carry):
            d = distance(k)
            kv_copy(from_along(d), order, d, side).wait_recv()
            kv_copy(from_along(d), order, depth_z + d, side).start()
            return carry

        loop(depth_z, one, 0)

    def relayed(order, state):
        def one(k, carry):
            d = distance(k)
            kv_copy(side_of(d), order, depth_z + d, side).wait_recv()
            return carry

        loop(depth_z, one, 0)
        return absorb_line(side_of, order, [], state)

    last = len(orders) - 1
    for order in range(last + 1):
        relay(order)
        if order > 0:
            state = relayed(order - 1, state)
        kv_copy(side, order, 0, side).wait_recv()
        state = absorb_line(from_along, order, [held(side, order)], state)
    state = relayed(last, state)

    _, total, summed = state
    ratio = summed / total
    mixed = ratio[:rows] - mix_in[...] * ratio[rows:]
    normed = (
        mixed * lax.rsqrt(jnp.mean(mixed * mixed, axis=-1, keepdims=True) + epsilon) * gain_in[...]
    )
    heads = normed.astype(jnp.bfloat16).reshape(groups, PIECES, 2, half, 2 * HEAD)
    for device in range(tp):
        for r in range(PIECES):
            hsend[device, r * half : (r + 1) * half, :] = heads[device // 2, r, device % 2]
    head_sends = []
    for d in range(1, tp):
        target = lax.rem(me_tp + d, tp)
        cp = pltpu.make_async_remote_copy(
            src_ref=hsend.at[target], dst_ref=hrecv.at[me_tp],
            send_sem=hs_sems.at[d], recv_sem=hr_sems.at[d],
            device_id={"tp": target}, device_id_type=MESH,
        )
        cp.start()
        head_sends.append(cp)
    hrecv[me_tp] = hsend[me_tp]
    for cp in head_sends:
        cp.wait_recv()
    joined = jnp.concatenate([hrecv[h] for h in range(tp)], axis=1)
    out[...] = jnp.dot(joined, wov[...], preferred_element_type=jnp.float32).astype(out.dtype)

    for cp in first_sends + forwards + head_sends:
        cp.wait_send()

    for order in range(last + 1):

        def drain(i, carry):
            kv_copy(me_sp, order, i, side).wait_send()
            return carry

        lax.fori_loop(0, depth_z, drain, 0)
        lax.fori_loop(depth_z + 1, 2 * depth_z, drain, 0)


def per_device(
    sp, tp,
    tokens, query_one, query_two, key_one, key_two, value_weight, mixing, out_weight, head_gain
):
    own_rows, depth = tokens.shape
    rows = own_rows * tp
    assert query_one.shape[1] == HEAD
    any_spec = pl.BlockSpec(memory_space=pl.ANY)
    vmem = pl.BlockSpec(memory_space=pltpu.VMEM)
    dma = pltpu.SemaphoreType.DMA
    bf16 = jnp.bfloat16
    return pl.pallas_call(
        functools.partial(kernel, sp, tp),
        out_shape=pltpu.VMEM((own_rows, out_weight.shape[1]), bf16),
        in_specs=[any_spec] * 6 + [any_spec] * 3,
        out_specs=vmem,
        scratch_shapes=[
            pltpu.VMEM((tp, own_rows, depth), bf16),
            pltpu.VMEM((4 * HEAD, depth), bf16),
            pltpu.VMEM((depth, 2 * HEAD), bf16),
            pltpu.VMEM(out_weight.shape, bf16),
            pltpu.VMEM((2, rows, 2 * HEAD), jnp.float32),
            pltpu.VMEM((sp, tp // 2, PIECES, own_rows, 4 * HEAD), bf16),
            pltpu.VMEM((2, rows, 2 * HEAD), bf16),
            pltpu.VMEM((tp, own_rows, 2 * HEAD), bf16),
            pltpu.VMEM((tp, own_rows, 2 * HEAD), bf16),
            dma((9,)),
            dma((tp // 2, PIECES)),
            dma((tp // 2, PIECES)),
            dma((tp // 2, PIECES)),
            dma((tp // 2, PIECES)),
            dma((1 + PIECES * (tp // 2 - 1), sp)),
            dma((1 + PIECES * (tp // 2 - 1), sp)),
            dma((tp,)),
            dma((tp,)),
            pltpu.SemaphoreType.REGULAR((2,)),
            pltpu.VMEM((1, 1), jnp.float32),
            pltpu.VMEM((1, 2 * HEAD), jnp.float32),
        ],
        compiler_params=pltpu.CompilerParams(
            collective_id=0, has_side_effects=True, vmem_limit_bytes=56 * 1024 * 1024
        ),
    )(
        tokens, query_one.T, query_two.T, key_one.T, key_two.T, value_weight,
        mixing.reshape(1, 1), out_weight, head_gain.reshape(1, -1),
    )


def solution(mesh):
    in_specs = (
        P(("sp", "tp"), None),
        P(None, "tp"),
        P(None, "tp"),
        P(None, "tp"),
        P(None, "tp"),
        P(None, "tp"),
        P("tp"),
        P(),
        P(),
    )
    out_specs = P(("sp", "tp"), None)
    return jax.shard_map(
        functools.partial(per_device, mesh.shape["sp"], mesh.shape["tp"]),
        mesh=mesh, in_specs=in_specs, out_specs=out_specs, check_vma=False,
    )
```

```python
import functools
import math

import jax
import jax.numpy as jnp
from jax import lax
from jax.experimental import pallas as pl
from jax.experimental.pallas import tpu as pltpu
from jax.sharding import PartitionSpec as P

HEAD = 64
GRID_W = 64
QUARTER = HEAD // 4

epsilon = 1e-06
theta_base = 10000.0
floor_value = -1e30
MESH = pl.DeviceIdType.MESH
NT = (((1,), (1,)), ((), ()))
PIECES = 2


def rotary_tables(start, rows, own_rows):
    shape = (rows, 2 * HEAD)
    lane = lax.broadcasted_iota(jnp.int32, shape, 1)
    index = lax.broadcasted_iota(jnp.int32, shape, 0)
    half = own_rows // PIECES
    device = 2 * (index // (2 * own_rows)) + (index % own_rows) // half
    piece = (index % (2 * own_rows)) // own_rows
    token = start + device * own_rows + piece * half + index % half
    entry = lane % QUARTER
    freqs = jnp.zeros(shape, jnp.float32)
    for j in range(QUARTER):
        freqs = jnp.where(entry == j, jnp.float32(theta_base ** (-j / QUARTER)), freqs)
    by_row = (lane % HEAD) < 2 * QUARTER
    position = jnp.where(by_row, token // GRID_W, token % GRID_W).astype(jnp.float32)
    angle = position * freqs
    first = (lane % (2 * QUARTER)) < QUARTER
    sine = jnp.sin(angle)
    return jnp.cos(angle), jnp.where(first, -sine, sine)


def turn(field, cosine, sine):
    lane = lax.broadcasted_iota(jnp.int32, field.shape, 1)
    first = (lane % (2 * QUARTER)) < QUARTER
    width = field.shape[1]
    other = jnp.where(
        first, pltpu.roll(field, width - QUARTER, 1), pltpu.roll(field, QUARTER, 1)
    )
    return field * cosine + other * sine


def kernel(
    sp, tp,
    tokens, wq1, wq2, wk1, wk2, wv, mixing, wo, gain, out,
    tok, wqk, wvv, wov, tables, kv, qbuf, hsend, hrecv,
    load_sems, tsend, trecv, fsend, frecv, ksend, krecv, hs_sems, hr_sems, ready, mix_in, gain_in,
):
    own_rows, depth = tokens.shape
    rows = own_rows * tp
    groups = tp // 2
    me_tp = lax.axis_index("tp")
    me_sp = lax.axis_index("sp")
    partner = me_tp + 1 - 2 * (me_tp % 2)
    half = own_rows // PIECES
    pair = 2 * own_rows
    me_chip = me_tp // 2
    orders = [(0, None)] + [(g, r) for g in range(1, groups) for r in range(PIECES)]

    depth_z = sp // 2
    me_z = me_sp // 2
    side = me_sp + 1 - 2 * (me_sp % 2)
    barrier = pltpu.get_barrier_semaphore()
    has_left = jnp.minimum(me_z, 1)
    has_right = jnp.minimum(depth_z - 1 - me_z, 1)

    def signal_line(left_sem, right_sem):
        @pl.when(me_z > 0)
        def _():
            pl.semaphore_signal(right_sem, inc=1, device_id={"sp": me_sp - 2}, device_id_type=MESH)

        @pl.when(me_z < depth_z - 1)
        def _():
            pl.semaphore_signal(left_sem, inc=1, device_id={"sp": me_sp + 2}, device_id_type=MESH)

    for d in range(1, tp):
        pl.semaphore_signal(barrier, inc=1, device_id={"tp": lax.rem(me_tp + d, tp)}, device_id_type=MESH)
    pl.semaphore_signal(barrier, inc=1, device_id={"sp": side}, device_id_type=MESH)
    signal_line(barrier, barrier)
    tok_load = pltpu.make_async_copy(tokens, tok.at[me_tp], load_sems.at[0])
    tok_load.start()
    loads = []
    for i, w in enumerate((wq1, wq2, wk1, wk2)):
        loads.append(pltpu.make_async_copy(w, wqk.at[pl.ds(i * HEAD, HEAD)], load_sems.at[1 + i]))
    loads.append(pltpu.make_async_copy(wv, wvv, load_sems.at[5]))
    for c in loads:
        c.start()
    wo_load = pltpu.make_async_copy(wo, wov, load_sems.at[6])
    small = [
        pltpu.make_async_copy(mixing, mix_in, load_sems.at[7]),
        pltpu.make_async_copy(gain, gain_in, load_sems.at[8]),
    ]
    for c in small:
        c.start()

    pl.semaphore_wait(barrier, tp + has_left + has_right)

    def send(slot, c, target, s_sem, r_sem):
        part = tok.at[slot, pl.ds(c * half, half)]
        return pltpu.make_async_remote_copy(
            src_ref=part, dst_ref=part, send_sem=s_sem, recv_sem=r_sem,
            device_id={"tp": target}, device_id_type=MESH,
        )

    def send_whole(slot):
        return pltpu.make_async_remote_copy(
            src_ref=tok.at[slot], dst_ref=tok.at[slot], send_sem=tsend.at[0, 0], recv_sem=trecv.at[0, 0],
            device_id={"tp": partner}, device_id_type=MESH,
        )

    def peer(g):
        return lax.rem(me_tp + 2 * g, tp)

    if depth_z > 2:
        signal_line(ready.at[0], ready.at[1])
    tok_load.wait()
    first_sends, forwards = [], []
    cp = send_whole(me_tp)
    cp.start()
    first_sends.append(cp)
    for c in range(PIECES):
        for g in range(1, groups):
            cp = send(me_tp, c, peer(g), tsend.at[g, c], trecv.at[g, c])
            cp.start()
            first_sends.append(cp)

    cosine, sine = rotary_tables(me_sp * rows, rows, own_rows)
    tables[0] = cosine
    tables[1] = sine

    def wait_line():
        @pl.when(me_z > 0)
        def _():
            pl.semaphore_wait(ready.at[0], 1)

        @pl.when(me_z < depth_z - 1)
        def _():
            pl.semaphore_wait(ready.at[1], 1)

    def pass_on(_, carry):
        wait_line()
        signal_line(ready.at[0], ready.at[1])
        return carry

    if depth_z > 3:
        lax.fori_loop(0, depth_z - 3, pass_on, 0)
    for c in loads + small:
        c.wait()
    wo_load.start()

    def chip_of(order):
        return lax.rem(me_chip + groups - orders[order][0], groups)

    def held(slot, order):
        piece = orders[order][1]
        if piece is None:
            return kv.at[slot, chip_of(order)]
        return kv.at[slot, chip_of(order), piece]

    def kv_copy(slot, order, i, device):
        return pltpu.make_async_remote_copy(
            src_ref=held(slot, order), dst_ref=held(slot, order),
            send_sem=ksend.at[order, i], recv_sem=krecv.at[order, i],
            device_id={"sp": device}, device_id_type=MESH,
        )

    upper = (2 * me_z) // depth_z

    def distance(k):
        return upper * k + (1 - upper) * (depth_z - k)

    def along(d):
        return 2 * lax.rem(me_z + d, depth_z) + me_sp % 2

    def from_along(d):
        return 2 * lax.rem(me_z + depth_z - d, depth_z) + me_sp % 2

    def loop(count, body, state):
        if count <= 8:
            for k in range(1, count):
                state = body(k, state)
            return state
        return lax.fori_loop(1, count, body, state)

    def finish(order):
        chip = chip_of(order)
        piece = orders[order][1]
        pieces = range(PIECES) if piece is None else (piece,)
        x = jnp.concatenate(
            [
                tok[pl.ds(2 * chip, 2), r * half : (r + 1) * half, :].reshape(own_rows, depth)
                for r in pieces
            ],
            axis=0,
        )
        count = x.shape[0]
        qk = lax.dot_general(x, wqk[...], NT, preferred_element_type=jnp.float32)
        values = jnp.dot(x, wvv[...], preferred_element_type=jnp.float32)
        start = pl.multiple_of(chip * pair + pieces[0] * own_rows, own_rows)
        where = pl.ds(start, count)
        cosine = tables[0, where, :]
        sine = tables[1, where, :]
        keys = turn(qk[:, 2 * HEAD :], cosine, sine).astype(jnp.bfloat16)
        values = values.astype(jnp.bfloat16)
        for i, r in enumerate(pieces):
            kv[me_sp, chip, r, :, : 2 * HEAD] = keys[i * own_rows : (i + 1) * own_rows]
            kv[me_sp, chip, r, :, 2 * HEAD :] = values[i * own_rows : (i + 1) * own_rows]

        if order == 0 and depth_z > 2:
            wait_line()

        def start_line(k, carry):
            d = distance(k)
            kv_copy(me_sp, order, d, along(d)).start()
            return carry

        loop(depth_z, start_line, 0)
        kv_copy(me_sp, order, 0, side).start()
        queries = turn(qk[:, : 2 * HEAD], cosine, sine)
        lane = lax.broadcasted_iota(jnp.int32, queries.shape, 1)
        qbuf[0, where, :] = jnp.where(lane < HEAD, queries, 0.0).astype(jnp.bfloat16)
        qbuf[1, where, :] = jnp.where(lane < HEAD, 0.0, queries).astype(jnp.bfloat16)

    send_whole(partner).wait_recv()
    finish(0)
    for order in range(1, len(orders)):
        g, r = orders[order]
        slot = 2 * chip_of(order) + me_tp % 2
        other = 2 * chip_of(order) + partner % 2
        send(slot, r, partner, tsend.at[g, r], trecv.at[g, r]).wait_recv()
        cp = send(slot, r, partner, fsend.at[g, r], frecv.at[g, r])
        cp.start()
        forwards.append(cp)
        send(other, r, partner, fsend.at[g, r], frecv.at[g, r]).wait_recv()
        finish(order)

    both = qbuf[...].reshape(2 * rows, 2 * HEAD)

    def absorb(blocks, state):
        peak, total, summed = state
        block = jnp.concatenate([b[...].reshape(-1, 4 * HEAD) for b in blocks], axis=0)
        k = block[:, : 2 * HEAD]
        v = block[:, 2 * HEAD :]
        scores = lax.dot_general(both, k, NT, preferred_element_type=jnp.float32) * HEAD ** (-0.5)
        new_peak = jnp.maximum(peak, jnp.max(scores, axis=1, keepdims=True))
        factor = jnp.exp(peak - new_peak)
        weights = jnp.exp(scores - new_peak)
        total = total * factor + jnp.sum(weights, axis=1, keepdims=True)
        summed = summed * factor + jnp.dot(
            weights.astype(jnp.bfloat16), v, preferred_element_type=jnp.float32
        )
        return new_peak, total, summed

    def absorb_line(sources, order, also, state):
        if depth_z <= 8:
            line = [held(sources(distance(k)), order) for k in range(1, depth_z)]
            return absorb(line + also, state)
        if also:
            state = absorb(also, state)
        return lax.fori_loop(
            1, depth_z, lambda k, s: absorb([held(sources(distance(k)), order)], s), state
        )

    def side_of(d):
        slot = from_along(d)
        return slot + 1 - 2 * (slot % 2)

    state = (
        jnp.full((2 * rows, 1), floor_value, jnp.float32),
        jnp.zeros((2 * rows, 1), jnp.float32),
        jnp.zeros((2 * rows, 2 * HEAD), jnp.float32),
    )
    state = absorb([kv.at[me_sp]], state)

    def relay(order):
        def one(k, carry):
            d = distance(k)
            kv_copy(from_along(d), order, d, side).wait_recv()
            kv_copy(from_along(d), order, depth_z + d, side).start()
            return carry

        loop(depth_z, one, 0)

    def relayed(order, state):
        def one(k, carry):
            d = distance(k)
            kv_copy(side_of(d), order, depth_z + d, side).wait_recv()
            return carry

        loop(depth_z, one, 0)
        return absorb_line(side_of, order, [], state)

    last = len(orders) - 1
    for order in range(last + 1):
        relay(order)
        if order > 0:
            state = relayed(order - 1, state)
        kv_copy(side, order, 0, side).wait_recv()
        state = absorb_line(from_along, order, [held(side, order)], state)
    state = relayed(last, state)

    _, total, summed = state
    ratio = summed / total
    mixed = ratio[:rows] - mix_in[...] * ratio[rows:]
    normed = (
        mixed * lax.rsqrt(jnp.mean(mixed * mixed, axis=-1, keepdims=True) + epsilon) * gain_in[...]
    )
    heads = normed.astype(jnp.bfloat16).reshape(groups, PIECES, 2, half, 2 * HEAD)
    for device in range(tp):
        for r in range(PIECES):
            hsend[device, r * half : (r + 1) * half, :] = heads[device // 2, r, device % 2]
    head_sends = []
    for d in range(1, tp):
        target = lax.rem(me_tp + d, tp)
        cp = pltpu.make_async_remote_copy(
            src_ref=hsend.at[target], dst_ref=hrecv.at[me_tp],
            send_sem=hs_sems.at[d], recv_sem=hr_sems.at[d],
            device_id={"tp": target}, device_id_type=MESH,
        )
        cp.start()
        head_sends.append(cp)
    hrecv[me_tp] = hsend[me_tp]
    wo_load.wait()
    for cp in head_sends:
        cp.wait_recv()
    joined = jnp.concatenate([hrecv[h] for h in range(tp)], axis=1)
    out[...] = jnp.dot(joined, wov[...], preferred_element_type=jnp.float32).astype(out.dtype)

    for cp in first_sends + forwards + head_sends:
        cp.wait_send()

    for order in range(last + 1):

        def drain(i, carry):
            kv_copy(me_sp, order, i, side).wait_send()
            return carry

        lax.fori_loop(0, depth_z, drain, 0)
        lax.fori_loop(depth_z + 1, 2 * depth_z, drain, 0)


def per_device(
    sp, tp,
    tokens, query_one, query_two, key_one, key_two, value_weight, mixing, out_weight, head_gain
):
    own_rows, depth = tokens.shape
    rows = own_rows * tp
    assert query_one.shape[1] == HEAD
    any_spec = pl.BlockSpec(memory_space=pl.ANY)
    vmem = pl.BlockSpec(memory_space=pltpu.VMEM)
    dma = pltpu.SemaphoreType.DMA
    bf16 = jnp.bfloat16
    return pl.pallas_call(
        functools.partial(kernel, sp, tp),
        out_shape=pltpu.VMEM((own_rows, out_weight.shape[1]), bf16),
        in_specs=[any_spec] * 6 + [any_spec] * 3,
        out_specs=vmem,
        scratch_shapes=[
            pltpu.VMEM((tp, own_rows, depth), bf16),
            pltpu.VMEM((4 * HEAD, depth), bf16),
            pltpu.VMEM((depth, 2 * HEAD), bf16),
            pltpu.VMEM(out_weight.shape, bf16),
            pltpu.VMEM((2, rows, 2 * HEAD), jnp.float32),
            pltpu.VMEM((sp, tp // 2, PIECES, own_rows, 4 * HEAD), bf16),
            pltpu.VMEM((2, rows, 2 * HEAD), bf16),
            pltpu.VMEM((tp, own_rows, 2 * HEAD), bf16),
            pltpu.VMEM((tp, own_rows, 2 * HEAD), bf16),
            dma((9,)),
            dma((tp // 2, PIECES)),
            dma((tp // 2, PIECES)),
            dma((tp // 2, PIECES)),
            dma((tp // 2, PIECES)),
            dma((1 + PIECES * (tp // 2 - 1), sp)),
            dma((1 + PIECES * (tp // 2 - 1), sp)),
            dma((tp,)),
            dma((tp,)),
            pltpu.SemaphoreType.REGULAR((2,)),
            pltpu.VMEM((1, 1), jnp.float32),
            pltpu.VMEM((1, 2 * HEAD), jnp.float32),
        ],
        compiler_params=pltpu.CompilerParams(
            collective_id=0, has_side_effects=True, vmem_limit_bytes=56 * 1024 * 1024
        ),
    )(
        tokens, query_one.T, query_two.T, key_one.T, key_two.T, value_weight,
        mixing.reshape(1, 1), out_weight, head_gain.reshape(1, -1),
    )


def solution(mesh):
    in_specs = (
        P(("sp", "tp"), None),
        P(None, "tp"),
        P(None, "tp"),
        P(None, "tp"),
        P(None, "tp"),
        P(None, "tp"),
        P("tp"),
        P(),
        P(),
    )
    out_specs = P(("sp", "tp"), None)
    return jax.shard_map(
        functools.partial(per_device, mesh.shape["sp"], mesh.shape["tp"]),
        mesh=mesh, in_specs=in_specs, out_specs=out_specs, check_vma=False,
    )
```
